32 devices in a mesh: fs: 8 (over z, y), tp: 4 (over x, core).
Axes of the slice: x: 2, y: 2, z: 4, core: 2. Of those that a mesh axis runs over, the one named last changes fastest.
Arguments:
- query_one: bfloat16 [5120, 1024], P('fs', 'tp'), as said below
- key_one: bfloat16 [5120, 1024], P('fs', 'tp'), as said below
- query_two: bfloat16 [5120, 1024], P('fs', 'tp'), as said below
- key_two: bfloat16 [5120, 1024], P('fs', 'tp'), as said below
- values: bfloat16 [5120, 2048], P('fs', 'tp'), may hold values from -6 to 6
- mix_ratio: float32 [8], P('tp'), may hold values from 0.3 to 0.8
- head_gain: float32 [256], replicated, may hold values from 0.1 to 1.9
- cotangent: bfloat16 [5120, 2048], P('fs', 'tp'), may hold values from -0.3125 to 0.3125
- left_roots: bfloat16 [2048, 2048], P('fs'), as said below
- right_roots: bfloat16 [2048, 256], P('tp'), as said below
- weight: float32 [2048, 2048], P('fs', 'tp'), may hold values from -3 to 3
- momentum: float32 [2048, 2048], P('fs', 'tp'), as said below
Outputs:
- update_step: float32 [2048, 2048], P('fs', 'tp')
- weight_new: float32 [2048, 2048], P('fs', 'tp')
- momentum_new: float32 [2048, 2048], P('fs', 'tp')
- weight_copy: bfloat16 [2048, 2048], P(None, 'tp')
The draws below stay inside these ranges and needn't reach their ends.
Inputs may be any that keep to these rules, and one draw needn't show every extreme that they name: `query_one`: Real-valued. `key_one`: Real-valued. `query_two`: Real-valued. `key_two`: Real-valued. `left_roots`: Real-valued. `right_roots`: Real-valued. `momentum`: Real-valued.
All inputs are finite; a program needn't handle non-finite values.
Results may differ from the reference program's by a relative error of at most 0.0039.
Values may be sent and summed in bfloat16 or wider, within the bound.
A program may use at most 64 MiB of HBM per device.

```python
import jax
import jax.numpy as jnp
from jax import lax

D = 2048
HEADS = 8
DK = 128
DV = 256
TOK_DEV = 640
HV = 2048
TOKENS = 5120
N_FS = 8


def drawn(key, salt):
    base = jax.random.fold_in(key, salt)
    width = HEADS * DK
    query = 1.3 * jax.random.truncated_normal(jax.random.fold_in(base, 1), -6.0, 6.0, (TOKENS, width), jnp.float32)
    keys = 1.3 * jax.random.truncated_normal(jax.random.fold_in(base, 2), -6.0, 6.0, (TOKENS, width), jnp.float32)
    return (query, keys)


def draw_query_one(key, part):
    return drawn(key, 11)[0].astype(jnp.bfloat16)


def draw_key_one(key, part):
    return drawn(key, 11)[1].astype(jnp.bfloat16)


def draw_query_two(key, part):
    return drawn(key, 12)[0].astype(jnp.bfloat16)


def draw_key_two(key, part):
    return drawn(key, 12)[1].astype(jnp.bfloat16)


def roots(key, count, size):
    noise = jax.random.normal(jax.random.fold_in(key, 21), (count, size, size), jnp.float32)
    symmetric = (noise + jnp.swapaxes(noise, 1, 2)) * 0.5 / (2.0 * size) ** 0.5
    diagonal = jax.random.uniform(jax.random.fold_in(key, 22), (count, size), jnp.float32, 1.0, 2.0)
    return symmetric + diagonal[:, :, None] * jnp.eye(size, dtype=jnp.float32)[None, :, :]


def draw_left_roots(key, part):
    return roots(key, 1, D).reshape(D, D).astype(jnp.bfloat16)


def draw_right_roots(key, part):
    return roots(key, HEADS, DV).reshape(HEADS * DV, DV).astype(jnp.bfloat16)


def draw_momentum(key, part):
    rows = 0.3 * (1.0 + 4.0 * jnp.arange(D, dtype=jnp.float32) / D)
    columns = 1.0 + 2.0 * jnp.arange(HV, dtype=jnp.float32) / HV
    base = jax.random.normal(key, (D, HV), jnp.float32)
    scales = rows[:, None] * columns[None, :]
    return base * scales


def spiked(result, own_key, source, target, blocks, factor):
    def block_of(axis_at):
        return (jnp.arange(result.shape[axis_at]) // (result.shape[axis_at] // blocks)).reshape((-1,) + (1,) * (result.ndim - 1 - axis_at))

    first = jax.random.permutation(own_key, blocks)[block_of(target)]
    other_side = (block_of(target) + blocks // 2) % blocks
    return jnp.where((block_of(source) == first) | (block_of(source) == other_side), factor * result, result)


def shard_levels(rng, extent, split, smallest, largest):
    factor_of = 1.0
    for dim, blocks in split:
        heights = jax.random.uniform(jax.random.fold_in(jax.random.fold_in(rng, 6), dim), (blocks,), jnp.float32, smallest / len(split), largest / len(split))
        factor_of = factor_of * jnp.repeat(jnp.exp(heights), extent[dim] // blocks).reshape((-1,) + (1,) * (len(extent) - 1 - dim))
    return factor_of


def gaussian(stream_key, dims, deviation, most, split=(), kind=jnp.bfloat16):
    level = shard_levels(stream_key, dims, split, -0.22, 0.18) if split else 1.0
    result = jax.random.normal(stream_key, dims, jnp.float32) * deviation * level
    return jnp.minimum(jnp.maximum(result, -most), most).astype(kind)


def noise_with(own_key, extent, spread, bound, split, heavy, kind=jnp.bfloat16):
    drawn = spread * jax.random.normal(own_key, extent, jnp.float32)
    if split:
        drawn = drawn * shard_levels(own_key, extent, split, -0.22, 0.18)
    return jnp.clip(spiked(drawn, jax.random.fold_in(own_key, 3), *heavy), -bound, bound).astype(kind)


def setup_inputs(seed: int = 0) -> dict:
    key_of = jax.random.split(jax.random.key(seed), 13)
    return {
        "query_one": draw_query_one(jax.random.fold_in(key_of[12], 71), 0),
        "key_one": draw_key_one(jax.random.fold_in(key_of[12], 71), 0),
        "query_two": draw_query_two(jax.random.fold_in(key_of[12], 71), 0),
        "key_two": draw_key_two(jax.random.fold_in(key_of[12], 71), 0),
        "values": gaussian(key_of[4], (TOKENS, HV), 1.0, 6.0, ((0, 8), (1, 4))),
        "mix_ratio": jnp.clip(0.3 + 0.5 * jax.random.uniform(key_of[5], (HEADS,), jnp.float32) ** shard_levels(key_of[5], (HEADS,), ((0, 4),), -0.2, 0.2), 0.3, 0.8),
        "head_gain": jnp.clip(1.0 + 0.18 * jax.random.normal(key_of[6], (DV,), jnp.float32), 0.1, 1.9),
        "cotangent": noise_with(key_of[7], (TOKENS, D), ((TOK_DEV * N_FS) ** -0.5), 0.3125, ((0, 8), (1, 4)), (0, 1, 8, 2.0)),
        "left_roots": draw_left_roots(jax.random.fold_in(key_of[12], 71), 0),
        "right_roots": draw_right_roots(jax.random.fold_in(key_of[12], 71), 0),
        "weight": gaussian(key_of[10], (D, HV), 0.5, 3.0, ((0, 8), (1, 4)), jnp.float32),
        "momentum": draw_momentum(jax.random.fold_in(key_of[12], 71), 0),
    }


epsilon = 1e-06
momentum_decay = 0.8
clip_level = 0.5
weight_decay = 0.2
step_rate = 0.1

def attend(query_one, key_one, query_two, key_two, values, mix_ratio, head_gain):
    count = TOKENS // TOK_DEV
    causal = jnp.tril(jnp.ones((TOK_DEV, TOK_DEV), dtype=bool))

    def probs(query, keys):
        scores = jnp.einsum('qhd,khd->hqk', query.astype(jnp.float32), keys.astype(jnp.float32)) * DK ** (-0.5)
        return jax.nn.softmax(jnp.where(causal, scores, -jnp.inf), axis=-1)

    def one_sequence(item):
        first_q, first_k, second_q, second_k, vals = item
        mixed = (probs(first_q, first_k) - mix_ratio[:, None, None] * probs(second_q, second_k)).astype(jnp.bfloat16)
        head_out = jnp.einsum('hqk,khd->qhd', mixed.astype(jnp.float32), vals.astype(jnp.float32))
        square = lax.optimization_barrier(jnp.mean(head_out * head_out, axis=-1, keepdims=True))
        normed = head_out * lax.rsqrt(square + epsilon) * head_gain
        return normed.astype(jnp.bfloat16).reshape(TOK_DEV, HV)
    shaped = (query_one.reshape(count, TOK_DEV, HEADS, DK), key_one.reshape(count, TOK_DEV, HEADS, DK), query_two.reshape(count, TOK_DEV, HEADS, DK), key_two.reshape(count, TOK_DEV, HEADS, DK), values.reshape(count, TOK_DEV, HEADS, DV))
    return lax.map(one_sequence, shaped).reshape(TOKENS, HV)

def reference(query_one, key_one, query_two, key_two, values, mix_ratio, head_gain, cotangent, left_roots, right_roots, weight, momentum):
    attended = attend(query_one, key_one, query_two, key_two, values, mix_ratio, head_gain)
    gradient = jnp.dot(cotangent.T, attended, preferred_element_type=jnp.float32)
    left_done = jnp.dot(left_roots.astype(jnp.float32), gradient, precision=lax.Precision.HIGHEST, preferred_element_type=jnp.float32)
    right_full = right_roots.astype(jnp.float32).reshape(HEADS, DV, DV)
    preconditioned = jnp.einsum('dhc,hce->dhe', left_done.reshape(D, HEADS, DV), right_full, precision=lax.Precision.HIGHEST).reshape(D, HV)
    momentum_new = momentum_decay * momentum + (1.0 - momentum_decay) * preconditioned
    total = jnp.sum(momentum_new * momentum_new)
    factor = clip_level * lax.rsqrt(total / (D * HV) + epsilon)
    update_step = factor * momentum_new + weight_decay * weight
    weight_new = weight - step_rate * update_step
    return (update_step, weight_new, momentum_new, weight_new.astype(jnp.bfloat16))
```

```python
import functools

import jax
import jax.numpy as jnp
from jax import lax
from jax.experimental import pallas as pl
from jax.experimental.pallas import tpu as pltpu
from jax.sharding import PartitionSpec as P

epsilon = 1e-06
momentum_decay = 0.8
clip_level = 0.5
weight_decay = 0.2
step_rate = 0.1
MESH = pl.DeviceIdType.MESH


def steps(first, last, body):
    if last - first <= 8:
        for at in range(first, last):
            body(at)
    else:

        def one(at, carry):
            body(at)
            return carry

        lax.fori_loop(first, last, one, 0)


def update_kernel(n_fs, n_tp, heads, wire, *refs):
    cots = refs[:n_tp]
    (att, left, right, weight, momentum, gathered, prec, factor_ref,
     gpart, yrecv, ysum, zrecv, acc, gfull, mnew, sq_all,
     ys, yr, zs, zr, gzs, gzr, gys, gyr, wzs, wzr, wys, wyr, ss, sr) = refs[n_tp:]
    f = lax.axis_index("fs")
    t = lax.axis_index("tp")
    ny = 2
    nz = n_fs // ny
    z = f // ny
    y = f % ny
    other = 1 - y
    rows = left.shape[0]
    depth = left.shape[1]
    vw = right.shape[1]
    block = cots[0].shape[0]
    f32 = jnp.float32

    def flip(a, b):
        out, bit = 0, 1
        while bit < n_tp:
            out = out + bit * ((a // bit + b // bit) % 2)
            bit *= 2
        return out

    def part_rows(dest):
        start = dest * rows
        j = start // block
        return pl.ds(pl.multiple_of(flip(j, t) * block + (start - j * block), rows), rows)

    def rows_of(dest):
        return pl.ds(pl.multiple_of(dest * rows, rows), rows)

    def copy(src, dst, send, recv, fs):
        return pltpu.make_async_remote_copy(
            src_ref=src, dst_ref=dst, send_sem=send, recv_sem=recv, device_id={"fs": fs}, device_id_type=MESH
        )

    partner = z * ny + other

    def y_copy(h, zz):
        return copy(gpart.at[h, part_rows(zz * ny + other)], yrecv.at[h, zz], ys.at[h, zz], yr.at[h, zz], partner)

    def z_copy(h, zz, slot):
        return copy(ysum.at[h, zz], zrecv.at[h, slot], zs.at[h, zz], zr.at[h, slot], zz * ny + y)

    for h in range(heads):
        cols = pl.ds(h * vw, vw)
        for k in range(n_tp):
            gpart[h, pl.ds(k * block, block), :] = jnp.dot(
                cots[k][...], att[:, cols], preferred_element_type=f32
            ).astype(wire)
        steps(1, nz + 1, lambda s, h=h: y_copy(h, (z + s) % nz).start())

    for h in range(heads):

        def pair(s, h=h):
            zz = (z + s) % nz
            y_copy(h, zz).wait_recv()
            total = gpart[h, part_rows(zz * ny + y), :].astype(f32) + yrecv[h, zz].astype(f32)
            ysum[h, zz] = total.astype(wire)
            z_copy(h, zz, z).start()

        steps(1, nz, pair)
        y_copy(h, z).wait_recv()
        acc[h] = gpart[h, part_rows(f), :].astype(f32) + yrecv[h, z].astype(f32)

    def gather_z(buf, send, recv, h, zz, owner):
        own = buf.at[h, rows_of(owner * ny + y)]
        return copy(own, own, send.at[h, zz], recv.at[h, owner], zz * ny + y)

    def gather_y(buf, send, recv, h, owner, side):
        own = buf.at[h, rows_of(owner * ny + side)]
        return copy(own, own, send.at[h, owner], recv.at[h, owner], partner)

    def gather_start(buf, zsend, zrec, ysend, yrec, h):
        steps(1, nz, lambda s: gather_z(buf, zsend, zrec, h, (z + s) % nz, z).start())
        gather_y(buf, ysend, yrec, h, z, y).start()

    def gather_forward(buf, zsend, zrec, ysend, yrec, h):
        def one(s):
            zz = (z + s) % nz
            gather_z(buf, zsend, zrec, h, zz, zz).wait_recv()
            gather_y(buf, ysend, yrec, h, zz, y).start()

        steps(1, nz, one)

    def gather_wait(buf, zsend, zrec, ysend, yrec, h):
        steps(0, nz, lambda zz: gather_y(buf, ysend, yrec, h, zz, other).wait_recv())

    def gather_sent(buf, zsend, zrec, ysend, yrec, h):
        steps(1, nz, lambda s: gather_z(buf, zsend, zrec, h, (z + s) % nz, z).wait_send())
        steps(0, nz, lambda zz: gather_y(buf, ysend, yrec, h, zz, y).wait_send())

    gsems = (gzs, gzr, gys, gyr)
    wsems = (wzs, wzr, wys, wyr)
    for h in range(heads):

        def arrive(s, h=h):
            zz = (z + s) % nz
            z_copy(h, zz, zz).wait_recv()
            acc[h] += zrecv[h, zz].astype(f32)

        steps(1, nz, arrive)
        gfull[h, rows_of(f), :] = acc[h].astype(jnp.bfloat16)
        gather_start(gfull, *gsems, h)
    for h in range(heads):
        gather_forward(gfull, *gsems, h)

    square = jnp.zeros((1, vw), f32)
    for h in range(heads):
        cols = pl.ds(h * vw, vw)
        gather_wait(gfull, *gsems, h)
        done = jnp.dot(left[...], gfull[h], preferred_element_type=f32)
        high = done.astype(jnp.bfloat16)
        low = (done - high.astype(f32)).astype(jnp.bfloat16)
        root = right[pl.ds(h * vw, vw), :]
        made = jnp.dot(high, root, preferred_element_type=f32) + jnp.dot(low, root, preferred_element_type=f32)
        prec[:, cols] = made
        new = momentum_decay * momentum[:, cols] + (1.0 - momentum_decay) * made
        mnew[h] = new
        square = square + jnp.sum(new * new, axis=0, keepdims=True)

    n = n_fs * n_tp
    me = f * n_tp + t
    sq_all[me] = square

    def sq_copy(dest, owner):
        return pltpu.make_async_remote_copy(
            src_ref=sq_all.at[owner], dst_ref=sq_all.at[owner], send_sem=ss.at[dest], recv_sem=sr.at[owner],
            device_id={"fs": dest // n_tp, "tp": dest % n_tp}, device_id_type=MESH,
        )

    def each(body):
        def one(s, carry):
            body((me + s) % n)
            return carry

        lax.fori_loop(1, n, one, 0)

    each(lambda d: sq_copy(d, me).start())
    each(lambda d: sq_copy(d, d).wait_recv())
    total = jnp.sum(jnp.sum(sq_all[...], axis=0), axis=1, keepdims=True)
    entries = depth * heads * vw * n_tp
    factor = clip_level * lax.rsqrt(jnp.broadcast_to(total, (1, vw)) / entries + epsilon)
    factor_ref[...] = factor

    for h in range(heads):
        kept = weight[:, pl.ds(h * vw, vw)]
        step = factor * mnew[h] + weight_decay * kept
        gathered[h, rows_of(f), :] = (kept - step_rate * step).astype(jnp.bfloat16)
        gather_start(gathered, *wsems, h)
    for h in range(heads):
        gather_forward(gathered, *wsems, h)
    for h in range(heads):
        gather_wait(gathered, *wsems, h)
        steps(0, nz, lambda zz, h=h: y_copy(h, zz).wait_send())
        steps(1, nz, lambda s, h=h: z_copy(h, (z + s) % nz, z).wait_send())
        gather_sent(gfull, *gsems, h)
        gather_sent(gathered, *wsems, h)
    each(lambda d: sq_copy(d, me).wait_send())


def local(
    n_fs,
    n_tp,
    query_one,
    key_one,
    query_two,
    key_two,
    values,
    mix_ratio,
    head_gain,
    cotangent,
    left_roots,
    right_roots,
    weight,
    momentum,
):
    local_heads = mix_ratio.shape[0]
    tok_rows = query_one.shape[0]
    key_width = query_one.shape[1] // local_heads
    value_width = values.shape[1] // local_heads
    causal = jnp.tril(jnp.ones((tok_rows, tok_rows), dtype=bool))

    cots = {0: cotangent.T}
    bit = n_tp // 2
    while bit:
        perm = [(i, i ^ bit) for i in range(n_tp)]
        cots.update({k ^ bit: lax.ppermute(block, "tp", perm) for k, block in cots.items()})
        bit //= 2

    def probs(query, keys):
        scores = jnp.einsum(
            "qhd,khd->hqk",
            query.reshape(tok_rows, local_heads, key_width),
            keys.reshape(tok_rows, local_heads, key_width),
            preferred_element_type=jnp.float32,
        ) * key_width ** (-0.5)
        return jax.nn.softmax(jnp.where(causal, scores, -jnp.inf), axis=-1)

    mixed = (
        probs(query_one, key_one) - mix_ratio[:, None, None] * probs(query_two, key_two)
    ).astype(jnp.bfloat16)
    head_out = jnp.einsum(
        "hqk,khd->qhd",
        mixed,
        values.reshape(tok_rows, local_heads, value_width),
        preferred_element_type=jnp.float32,
    )
    square = jnp.mean(head_out * head_out, axis=-1, keepdims=True)
    attended = (head_out * lax.rsqrt(square + epsilon) * head_gain).astype(jnp.bfloat16)
    attended = attended.reshape(tok_rows, local_heads * value_width)

    rows, depth = left_roots.shape
    nz = n_fs // 2
    n = n_fs * n_tp
    wire = jnp.bfloat16 if n_fs <= 8 else jnp.float32
    vmem = pl.BlockSpec(memory_space=pltpu.VMEM)
    bf16, f32 = jnp.bfloat16, jnp.float32
    dma = pltpu.SemaphoreType.DMA
    gathered, prec, factor = pl.pallas_call(
        functools.partial(update_kernel, n_fs, n_tp, local_heads, wire),
        out_shape=(
            jax.ShapeDtypeStruct((local_heads, depth, value_width), bf16),
            jax.ShapeDtypeStruct(weight.shape, f32),
            jax.ShapeDtypeStruct((1, value_width), f32),
        ),
        in_specs=[vmem] * (n_tp + 5),
        out_specs=(vmem, vmem, vmem),
        scratch_shapes=[
            pltpu.VMEM((local_heads, depth, value_width), wire),
            pltpu.VMEM((local_heads, nz, rows, value_width), wire),
            pltpu.VMEM((local_heads, nz, rows, value_width), wire),
            pltpu.VMEM((local_heads, nz, rows, value_width), wire),
            pltpu.VMEM((local_heads, rows, value_width), f32),
            pltpu.VMEM((local_heads, depth, value_width), bf16),
            pltpu.VMEM((local_heads, rows, value_width), f32),
            pltpu.VMEM((n, 1, value_width), f32),
        ]
        + [dma((local_heads, nz))] * 12
        + [dma((n,))] * 2,
        compiler_params=pltpu.CompilerParams(has_side_effects=True, vmem_limit_bytes=56 * 1024 * 1024),
    )(*[cots[k] for k in range(n_tp)], attended, left_roots, right_roots, weight, momentum)
    factor = factor[:1, :1]
    momentum_new = momentum_decay * momentum + (1.0 - momentum_decay) * prec
    update_step = factor * momentum_new + weight_decay * weight
    weight_new = weight - step_rate * update_step
    weight_copy = jnp.swapaxes(gathered, 0, 1).reshape(depth, local_heads * value_width)
    return (update_step, weight_new, momentum_new, weight_copy)


def solution(mesh):
    in_specs = (
        P("fs", "tp"),
        P("fs", "tp"),
        P("fs", "tp"),
        P("fs", "tp"),
        P("fs", "tp"),
        P("tp"),
        P(),
        P("fs", "tp"),
        P("fs", None),
        P("tp", None),
        P("fs", "tp"),
        P("fs", "tp"),
    )
    out_specs = (P("fs", "tp"), P("fs", "tp"), P("fs", "tp"), P(None, "tp"))
    body = functools.partial(local, mesh.shape["fs"], mesh.shape["tp"])
    return jax.shard_map(body, mesh=mesh, in_specs=in_specs, out_specs=out_specs, check_vma=False)
```

```python
import functools

import jax
import jax.numpy as jnp
from jax import lax
from jax.experimental import pallas as pl
from jax.experimental.pallas import tpu as pltpu
from jax.sharding import PartitionSpec as P

epsilon = 1e-06
momentum_decay = 0.8
clip_level = 0.5
weight_decay = 0.2
step_rate = 0.1
MESH = pl.DeviceIdType.MESH


def steps(first, last, body):
    if last - first <= 8:
        for at in range(first, last):
            body(at)
    else:

        def one(at, carry):
            body(at)
            return carry

        lax.fori_loop(first, last, one, 0)


def update_kernel(n_fs, n_tp, heads, wire, *refs):
    (mix, q_one, k_one, q_two, k_two, values, gain, cot, left, right, weight, momentum,
     gathered, prec, factor_ref,
     att, cots, gpart, yrecv, ysum, zrecv, acc, gfull, mnew, sq_all,
     cs, cr, ys, yr, zs, zr, gzs, gzr, gys, gyr, wzs, wzr, wys, wyr, ss, sr) = refs
    f = lax.axis_index("fs")
    t = lax.axis_index("tp")
    ny = 2
    nz = n_fs // ny
    pz = nz // n_tp
    z = f // ny
    y = f % ny
    other = 1 - y
    rows = left.shape[0]
    depth = left.shape[1]
    vw = right.shape[1]
    block = cot.shape[0]
    tokens = cot.shape[1]
    f32 = jnp.float32

    def flip(a, b):
        out, bit = 0, 1
        while bit < n_tp:
            out = out + bit * ((a // bit + b // bit) % 2)
            bit *= 2
        return out

    def part_rows(dest):
        start = dest * rows
        j = start // block
        return pl.ds(pl.multiple_of(flip(j, t) * block + (start - j * block), rows), rows)

    def cot_copy(k, bit):
        src = cot if k == 0 else cots.at[k]
        return pltpu.make_async_remote_copy(
            src_ref=src, dst_ref=cots.at[k + bit], send_sem=cs.at[k + bit], recv_sem=cr.at[k + bit],
            device_id={"tp": flip(t, bit)}, device_id_type=MESH,
        )

    bits = []
    while 2 ** len(bits) < n_tp:
        bits.insert(0, 2 ** len(bits))
    for bit in bits:
        cot_copy(0, bit).start()

    key_width = q_one.shape[1] // heads
    tile = 128
    lanes = (((1,), (1,)), ((), ()))

    def attend(h):
        kcols = pl.ds(h * key_width, key_width)
        vcols = pl.ds(h * vw, vw)
        for first in range(0, tokens, tile):
            seen = first + tile
            causal = lax.broadcasted_iota(jnp.int32, (tile, seen), 1) <= first + lax.broadcasted_iota(
                jnp.int32, (tile, seen), 0
            )

            def probs(query, keys):
                scores = lax.dot_general(
                    query[pl.ds(first, tile), kcols], keys[pl.ds(0, seen), kcols], lanes, preferred_element_type=f32
                ) * key_width ** (-0.5)
                scores = jnp.where(causal, scores, -jnp.inf)
                grown = jnp.exp(scores - jnp.max(scores, axis=1, keepdims=True))
                return grown * (1.0 / jnp.sum(grown, axis=1, keepdims=True))

            mixed = (probs(q_one, k_one) - mix[h] * probs(q_two, k_two)).astype(jnp.bfloat16)
            out = jnp.dot(mixed, values[pl.ds(0, seen), vcols], preferred_element_type=f32)
            square = jnp.mean(out * out, axis=1, keepdims=True)
            att[pl.ds(first, tile), vcols] = (out * lax.rsqrt(square + epsilon) * gain[...]).astype(jnp.bfloat16)

    def rows_of(dest):
        return pl.ds(pl.multiple_of(dest * rows, rows), rows)

    def copy(src, dst, send, recv, fs):
        return pltpu.make_async_remote_copy(
            src_ref=src, dst_ref=dst, send_sem=send, recv_sem=recv, device_id={"fs": fs}, device_id_type=MESH
        )

    partner = z * ny + other

    def y_copy(h, zz):
        return copy(gpart.at[h, part_rows(zz * ny + other)], yrecv.at[h, zz], ys.at[h, zz], yr.at[h, zz], partner)

    def z_copy(h, zz, slot):
        return copy(ysum.at[h, zz], zrecv.at[h, slot], zs.at[h, zz], zr.at[h, slot], zz * ny + y)

    def zz_of(k, i):
        return flip(t, k) * pz + i

    def share(h, k):
        held = cot if k == 0 else cots.at[k]
        gpart[h, pl.ds(k * block, block), :] = jnp.dot(
            held[...], att[:, pl.ds(h * vw, vw)], preferred_element_type=f32
        ).astype(wire)
        steps(0, pz, lambda i: y_copy(h, zz_of(k, i)).start())

    def pairs(h, k):
        def pair(i):
            zz = zz_of(k, i)
            y_copy(h, zz).wait_recv()
            total = gpart[h, part_rows(zz * ny + y), :].astype(f32) + yrecv[h, zz].astype(f32)

            @pl.when(zz == z)
            def _():
                acc[h] = total

            @pl.when(zz != z)
            def _():
                ysum[h, zz] = total.astype(wire)
                z_copy(h, zz, z).start()

        steps(0, pz, pair)

    got = [0]

    def need(k):
        if k not in got:
            got.append(k)
            low = k & -k
            cot_copy(k - low, low).wait_recv()

    near = [0, 1]
    for h in range(heads):
        attend(h)
        for k in near:
            need(k)
            share(h, k)
    for k in near:
        pairs(0, k)
    order = list(near)
    ready = [0]
    for bit in bits:
        for k in list(ready):
            need(k)
            if k:
                cot_copy(k, bit).start()
            if k not in order:
                order.append(k)
                for h in range(heads):
                    share(h, k)
            ready.append(k + bit)
    for k in range(n_tp):
        if k not in order:
            order.append(k)
            need(k)
            for h in range(heads):
                share(h, k)
    for h in range(1, heads):
        for k in near:
            pairs(h, k)
    for h in range(heads):
        for k in order[len(near):]:
            pairs(h, k)

    def piece(buf, h, owner):
        if len(buf.shape) == 3:
            return buf.at[h, rows_of(owner)]
        return buf.at[rows_of(owner), pl.ds(h * vw, vw)]

    def gather_z(buf, send, recv, h, zz, owner):
        own = piece(buf, h, owner * ny + y)
        return copy(own, own, send.at[h, zz], recv.at[h, owner], zz * ny + y)

    def gather_y(buf, send, recv, h, owner, side):
        own = piece(buf, h, owner * ny + side)
        return copy(own, own, send.at[h, owner], recv.at[h, owner], partner)

    def gather_start(buf, zsend, zrec, ysend, yrec, h):
        steps(1, nz, lambda s: gather_z(buf, zsend, zrec, h, (z + s) % nz, z).start())
        gather_y(buf, ysend, yrec, h, z, y).start()

    def gather_forward(buf, zsend, zrec, ysend, yrec, h):
        def one(s):
            zz = (z + s) % nz
            gather_z(buf, zsend, zrec, h, zz, zz).wait_recv()
            gather_y(buf, ysend, yrec, h, zz, y).start()

        steps(1, nz, one)

    def gather_wait(buf, zsend, zrec, ysend, yrec, h):
        steps(0, nz, lambda zz: gather_y(buf, ysend, yrec, h, zz, other).wait_recv())

    def gather_sent(buf, zsend, zrec, ysend, yrec, h):
        steps(1, nz, lambda s: gather_z(buf, zsend, zrec, h, (z + s) % nz, z).wait_send())
        steps(0, nz, lambda zz: gather_y(buf, ysend, yrec, h, zz, y).wait_send())

    gsems = (gzs, gzr, gys, gyr)
    wsems = (wzs, wzr, wys, wyr)
    for h in range(heads):

        def arrive(s, h=h):
            zz = (z + s) % nz
            z_copy(h, zz, zz).wait_recv()
            acc[h] += zrecv[h, zz].astype(f32)

        steps(1, nz, arrive)
        gfull[h, rows_of(f), :] = acc[h].astype(jnp.bfloat16)
        gather_start(gfull, *gsems, h)
    for h in range(heads):
        gather_forward(gfull, *gsems, h)

    square = jnp.zeros((1, vw), f32)
    for h in range(heads):
        cols = pl.ds(h * vw, vw)
        gather_wait(gfull, *gsems, h)
        done = jnp.dot(left[...], gfull[h], preferred_element_type=f32)
        high = done.astype(jnp.bfloat16)
        low = (done - high.astype(f32)).astype(jnp.bfloat16)
        root = right[pl.ds(h * vw, vw), :]
        made = jnp.dot(high, root, preferred_element_type=f32) + jnp.dot(low, root, preferred_element_type=f32)
        prec[:, cols] = made
        new = momentum_decay * momentum[:, cols] + (1.0 - momentum_decay) * made
        mnew[h] = new
        square = square + jnp.sum(new * new, axis=0, keepdims=True)

    n = n_fs * n_tp
    me = f * n_tp + t
    sq_all[me] = square

    def sq_copy(dest, owner):
        return pltpu.make_async_remote_copy(
            src_ref=sq_all.at[owner], dst_ref=sq_all.at[owner], send_sem=ss.at[dest], recv_sem=sr.at[owner],
            device_id={"fs": dest // n_tp, "tp": dest % n_tp}, device_id_type=MESH,
        )

    def each(body):
        def one(s, carry):
            body((me + s) % n)
            return carry

        lax.fori_loop(1, n, one, 0)

    each(lambda d: sq_copy(d, me).start())
    each(lambda d: sq_copy(d, d).wait_recv())
    total = jnp.sum(jnp.sum(sq_all[...], axis=0), axis=1, keepdims=True)
    entries = depth * heads * vw * n_tp
    factor = clip_level * lax.rsqrt(jnp.broadcast_to(total, (1, vw)) / entries + epsilon)
    for h in range(heads):
        factor_ref[:, pl.ds(h * vw, vw)] = factor

    for h in range(heads):
        kept = weight[:, pl.ds(h * vw, vw)]
        step = factor * mnew[h] + weight_decay * kept
        gathered[rows_of(f), pl.ds(h * vw, vw)] = (kept - step_rate * step).astype(jnp.bfloat16)
        gather_start(gathered, *wsems, h)
    for h in range(heads):
        gather_forward(gathered, *wsems, h)
    for h in range(heads):
        gather_wait(gathered, *wsems, h)
        steps(0, nz, lambda zz, h=h: y_copy(h, zz).wait_send())
        steps(1, nz, lambda s, h=h: z_copy(h, (z + s) % nz, z).wait_send())
        gather_sent(gfull, *gsems, h)
        gather_sent(gathered, *wsems, h)
    each(lambda d: sq_copy(d, me).wait_send())
    held = [0]
    for bit in bits:
        for k in list(held):
            cot_copy(k, bit).wait_send()
            held.append(k + bit)


def local(
    n_fs,
    n_tp,
    query_one,
    key_one,
    query_two,
    key_two,
    values,
    mix_ratio,
    head_gain,
    cotangent,
    left_roots,
    right_roots,
    weight,
    momentum,
):
    local_heads = mix_ratio.shape[0]
    tok_rows = query_one.shape[0]
    value_width = values.shape[1] // local_heads
    block = cotangent.shape[1]

    rows, depth = left_roots.shape
    nz = n_fs // 2
    n = n_fs * n_tp
    wire = jnp.bfloat16 if n_fs <= 8 else jnp.float32
    vmem = pl.BlockSpec(memory_space=pltpu.VMEM)
    bf16, f32 = jnp.bfloat16, jnp.float32
    dma = pltpu.SemaphoreType.DMA
    gathered, prec, factor = pl.pallas_call(
        functools.partial(update_kernel, n_fs, n_tp, local_heads, wire),
        out_shape=(
            jax.ShapeDtypeStruct((depth, weight.shape[1]), bf16),
            jax.ShapeDtypeStruct(weight.shape, f32),
            jax.ShapeDtypeStruct((1, weight.shape[1]), f32),
        ),
        in_specs=[pl.BlockSpec(memory_space=pltpu.SMEM)] + [vmem] * 11,
        out_specs=(vmem, vmem, vmem),
        scratch_shapes=[
            pltpu.VMEM((tok_rows, weight.shape[1]), bf16),
            pltpu.VMEM((n_tp, block, tok_rows), bf16),
            pltpu.VMEM((local_heads, depth, value_width), wire),
            pltpu.VMEM((local_heads, nz, rows, value_width), wire),
            pltpu.VMEM((local_heads, nz, rows, value_width), wire),
            pltpu.VMEM((local_heads, nz, rows, value_width), wire),
            pltpu.VMEM((local_heads, rows, value_width), f32),
            pltpu.VMEM((local_heads, depth, value_width), bf16),
            pltpu.VMEM((local_heads, rows, value_width), f32),
            pltpu.VMEM((n, 1, value_width), f32),
        ]
        + [dma((n_tp,))] * 2
        + [dma((local_heads, nz))] * 12
        + [dma((n,))] * 2,
        compiler_params=pltpu.CompilerParams(has_side_effects=True, vmem_limit_bytes=56 * 1024 * 1024),
    )(
        mix_ratio, query_one, key_one, query_two, key_two, values, head_gain.reshape(1, -1), cotangent.T,
        left_roots, right_roots, weight, momentum,
    )
    momentum_new = momentum_decay * momentum + (1.0 - momentum_decay) * prec
    update_step = factor * momentum_new + weight_decay * weight
    weight_new = weight - step_rate * update_step
    return (update_step, weight_new, momentum_new, gathered)


def solution(mesh):
    in_specs = (
        P("fs", "tp"),
        P("fs", "tp"),
        P("fs", "tp"),
        P("fs", "tp"),
        P("fs", "tp"),
        P("tp"),
        P(),
        P("fs", "tp"),
        P("fs", None),
        P("tp", None),
        P("fs", "tp"),
        P("fs", "tp"),
    )
    out_specs = (P("fs", "tp"), P("fs", "tp"), P("fs", "tp"), P(None, "tp"))
    body = functools.partial(local, mesh.shape["fs"], mesh.shape["tp"])
    return jax.shard_map(body, mesh=mesh, in_specs=in_specs, out_specs=out_specs, check_vma=False)
```

```python
import functools

import jax
import jax.numpy as jnp
from jax import lax
from jax.experimental import pallas as pl
from jax.experimental.pallas import tpu as pltpu
from jax.sharding import PartitionSpec as P

epsilon = 1e-06
momentum_decay = 0.8
clip_level = 0.5
weight_decay = 0.2
step_rate = 0.1
MESH = pl.DeviceIdType.MESH


def steps(first, last, body):
    if last - first <= 8:
        for at in range(first, last):
            body(at)
    else:

        def one(at, carry):
            body(at)
            return carry

        lax.fori_loop(first, last, one, 0)


def update_kernel(n_fs, n_tp, heads, wire, *refs):
    (mix, q_one, k_one, q_two, k_two, values, gain, cot, left, right, weight, momentum,
     gathered, prec, factor_ref,
     att, cots, gpart, outgoing, incoming, gfull, mnew, sq_all,
     cs, cr, rs, rr, gs, gr, ws, wr, ss, sr) = refs
    f = lax.axis_index("fs")
    t = lax.axis_index("tp")
    side = n_fs // 2
    place = (f % 2) * (n_fs - 1 - f // 2) + (1 - f % 2) * (f // 2)
    rows = left.shape[0]
    depth = left.shape[1]
    vw = right.shape[1]
    block = cot.shape[0]
    tokens = cot.shape[1]
    f32 = jnp.float32

    def flip(a, b):
        out, bit = 0, 1
        while bit < n_tp:
            out = out + bit * ((a // bit + b // bit) % 2)
            bit *= 2
        return out

    def part_rows(dest):
        start = dest * rows
        j = start // block
        return pl.ds(pl.multiple_of(flip(j, t) * block + (start - j * block), rows), rows)

    def cot_copy(k, bit):
        src = cot if k == 0 else cots.at[k]
        return pltpu.make_async_remote_copy(
            src_ref=src, dst_ref=cots.at[k + bit], send_sem=cs.at[k + bit], recv_sem=cr.at[k + bit],
            device_id={"tp": flip(t, bit)}, device_id_type=MESH,
        )

    bits = []
    while 2 ** len(bits) < n_tp:
        bits.insert(0, 2 ** len(bits))
    for bit in bits:
        cot_copy(0, bit).start()

    key_width = q_one.shape[1] // heads
    tile = 128
    lanes = (((1,), (1,)), ((), ()))

    def attend(h):
        kcols = pl.ds(h * key_width, key_width)
        vcols = pl.ds(h * vw, vw)
        for first in range(0, tokens, tile):
            seen = first + tile
            causal = lax.broadcasted_iota(jnp.int32, (tile, seen), 1) <= first + lax.broadcasted_iota(
                jnp.int32, (tile, seen), 0
            )

            def probs(query, keys):
                scores = lax.dot_general(
                    query[pl.ds(first, tile), kcols], keys[pl.ds(0, seen), kcols], lanes, preferred_element_type=f32
                ) * key_width ** (-0.5)
                scores = jnp.where(causal, scores, -jnp.inf)
                grown = jnp.exp(scores - jnp.max(scores, axis=1, keepdims=True))
                return grown * (1.0 / jnp.sum(grown, axis=1, keepdims=True))

            mixed = (probs(q_one, k_one) - mix[h] * probs(q_two, k_two)).astype(jnp.bfloat16)
            out = jnp.dot(mixed, values[pl.ds(0, seen), vcols], preferred_element_type=f32)
            square = jnp.mean(out * out, axis=1, keepdims=True)
            att[pl.ds(first, tile), vcols] = (out * lax.rsqrt(square + epsilon) * gain[...]).astype(jnp.bfloat16)

    def rows_of(dest):
        return pl.ds(pl.multiple_of(dest * rows, rows), rows)

    def member(at):
        at = (at + n_fs) % n_fs
        back = at // side
        return 2 * (back * (n_fs - 1 - at) + (1 - back) * at) + back

    ways = ((0, 1), (1, -1))

    def hops(h, d):
        return side if (h + d) % 2 == 0 else n_fs - 1 - side

    def copy(src, dst, send, recv, sign):
        return pltpu.make_async_remote_copy(
            src_ref=src, dst_ref=dst, send_sem=send, recv_sem=recv, device_id={"fs": member(place + sign)},
            device_id_type=MESH,
        )

    def each_hop(body):
        short = n_fs - 1 - side

        def all_of(at):
            for h in range(heads):
                for d, sign in ways:
                    body(h, d, sign, at)

        steps(1, short, all_of)
        for h in range(heads):
            for d, sign in ways:
                if hops(h, d) > short and short >= 1:
                    body(h, d, sign, short)

    def sum_copy(h, d, sign, at):
        return copy(outgoing.at[d, h, at], incoming.at[d, h, at], rs.at[d, h, at], rr.at[d, h, at], sign)

    def sum_start(h):
        for d, sign in ways:
            outgoing[d, h, 0] = gpart[h, part_rows(member(place + sign * hops(h, d))), :].astype(wire)
            sum_copy(h, d, sign, 0).start()

    def sum_hop(h, d, sign, at):
        sum_copy(h, d, sign, at - 1).wait_recv()
        own = gpart[h, part_rows(member(place + sign * (hops(h, d) - at))), :]
        outgoing[d, h, at] = (own + incoming[d, h, at - 1].astype(f32)).astype(wire)
        sum_copy(h, d, sign, at).start()

    def sum_end(h):
        total = gpart[h, part_rows(f), :]
        for d, sign in ways:
            last = hops(h, d) - 1
            sum_copy(h, d, sign, last).wait_recv()
            total = total + incoming[d, h, last].astype(f32)
        return total

    def piece(buf, h, owner):
        if len(buf.shape) == 3:
            return buf.at[h, rows_of(owner)]
        return buf.at[rows_of(owner), pl.ds(h * vw, vw)]

    def pass_copy(buf, send, recv, h, d, sign, at, back=0):
        held = piece(buf, h, member(place - sign * (at + back)))
        return copy(held, held, send.at[d, h, at], recv.at[d, h, at], sign)

    def pass_start(buf, send, recv, h):
        for d, sign in ways:
            pass_copy(buf, send, recv, h, d, sign, 0).start()

    def pass_rest(buf, send, recv):
        def hop(h, d, sign, at):
            pass_copy(buf, send, recv, h, d, sign, at - 1, 1).wait_recv()
            pass_copy(buf, send, recv, h, d, sign, at).start()

        each_hop(hop)

    def pass_end(buf, send, recv, h):
        for d, sign in ways:
            pass_copy(buf, send, recv, h, d, sign, hops(h, d) - 1, 1).wait_recv()

    def all_sent(make):
        for h in range(heads):
            for d, sign in ways:
                steps(0, hops(h, d), lambda at, h=h, d=d, sign=sign: make(h, d, sign, at).wait_send())

    def share(h, k):
        held = cot if k == 0 else cots.at[k]
        gpart[h, pl.ds(k * block, block), :] = jnp.dot(
            held[...], att[:, pl.ds(h * vw, vw)], preferred_element_type=f32
        )

    got = [0]

    def need(k):
        if k not in got:
            got.append(k)
            low = k & -k
            cot_copy(k - low, low).wait_recv()

    for h in range(heads):
        attend(h)
    ready = [0]
    for bit in bits:
        for k in list(ready):
            need(k)
            if k:
                cot_copy(k, bit).start()
            ready.append(k + bit)
    for h in range(heads):
        for k in ready:
            need(k)
            share(h, k)
        sum_start(h)
    each_hop(sum_hop)
    for h in range(heads):
        gfull[h, rows_of(f), :] = sum_end(h).astype(jnp.bfloat16)
        pass_start(gfull, gs, gr, h)
    pass_rest(gfull, gs, gr)

    square = jnp.zeros((1, vw), f32)
    for h in range(heads):
        cols = pl.ds(h * vw, vw)
        pass_end(gfull, gs, gr, h)
        done = jnp.dot(left[...], gfull[h], preferred_element_type=f32)
        high = done.astype(jnp.bfloat16)
        low = (done - high.astype(f32)).astype(jnp.bfloat16)
        root = right[pl.ds(h * vw, vw), :]
        made = jnp.dot(high, root, preferred_element_type=f32) + jnp.dot(low, root, preferred_element_type=f32)
        prec[:, cols] = made
        new = momentum_decay * momentum[:, cols] + (1.0 - momentum_decay) * made
        mnew[h] = new
        square = square + jnp.sum(new * new, axis=0, keepdims=True)

    n = n_fs * n_tp
    me = f * n_tp + t
    sq_all[me] = square

    def sq_copy(dest, owner):
        return pltpu.make_async_remote_copy(
            src_ref=sq_all.at[owner], dst_ref=sq_all.at[owner], send_sem=ss.at[dest], recv_sem=sr.at[owner],
            device_id={"fs": dest // n_tp, "tp": dest % n_tp}, device_id_type=MESH,
        )

    def each(body):
        def one(s, carry):
            body((me + s) % n)
            return carry

        lax.fori_loop(1, n, one, 0)

    each(lambda d: sq_copy(d, me).start())
    each(lambda d: sq_copy(d, d).wait_recv())
    total = jnp.sum(jnp.sum(sq_all[...], axis=0), axis=1, keepdims=True)
    entries = depth * heads * vw * n_tp
    factor = clip_level * lax.rsqrt(jnp.broadcast_to(total, (1, vw)) / entries + epsilon)
    for h in range(heads):
        factor_ref[:, pl.ds(h * vw, vw)] = factor

    for h in range(heads):
        kept = weight[:, pl.ds(h * vw, vw)]
        step = factor * mnew[h] + weight_decay * kept
        gathered[rows_of(f), pl.ds(h * vw, vw)] = (kept - step_rate * step).astype(jnp.bfloat16)
        pass_start(gathered, ws, wr, h)
    pass_rest(gathered, ws, wr)
    for h in range(heads):
        pass_end(gathered, ws, wr, h)
    all_sent(sum_copy)
    all_sent(functools.partial(pass_copy, gfull, gs, gr))
    all_sent(functools.partial(pass_copy, gathered, ws, wr))
    each(lambda d: sq_copy(d, me).wait_send())
    held = [0]
    for bit in bits:
        for k in list(held):
            cot_copy(k, bit).wait_send()
            held.append(k + bit)


def local(
    n_fs,
    n_tp,
    query_one,
    key_one,
    query_two,
    key_two,
    values,
    mix_ratio,
    head_gain,
    cotangent,
    left_roots,
    right_roots,
    weight,
    momentum,
):
    local_heads = mix_ratio.shape[0]
    tok_rows = query_one.shape[0]
    value_width = values.shape[1] // local_heads
    block = cotangent.shape[1]

    rows, depth = left_roots.shape
    side = n_fs // 2
    n = n_fs * n_tp
    wire = jnp.bfloat16 if n_fs <= 8 else jnp.float32
    vmem = pl.BlockSpec(memory_space=pltpu.VMEM)
    bf16, f32 = jnp.bfloat16, jnp.float32
    dma = pltpu.SemaphoreType.DMA
    gathered, prec, factor = pl.pallas_call(
        functools.partial(update_kernel, n_fs, n_tp, local_heads, wire),
        out_shape=(
            jax.ShapeDtypeStruct((depth, weight.shape[1]), bf16),
            jax.ShapeDtypeStruct(weight.shape, f32),
            jax.ShapeDtypeStruct((1, weight.shape[1]), f32),
        ),
        in_specs=[pl.BlockSpec(memory_space=pltpu.SMEM)] + [vmem] * 11,
        out_specs=(vmem, vmem, vmem),
        scratch_shapes=[
            pltpu.VMEM((tok_rows, weight.shape[1]), bf16),
            pltpu.VMEM((n_tp, block, tok_rows), bf16),
            pltpu.VMEM((local_heads, depth, value_width), f32),
            pltpu.VMEM((2, local_heads, side, rows, value_width), wire),
            pltpu.VMEM((2, local_heads, side, rows, value_width), wire),
            pltpu.VMEM((local_heads, depth, value_width), bf16),
            pltpu.VMEM((local_heads, rows, value_width), f32),
            pltpu.VMEM((n, 1, value_width), f32),
        ]
        + [dma((n_tp,))] * 2
        + [dma((2, local_heads, side))] * 6
        + [dma((n,))] * 2,
        compiler_params=pltpu.CompilerParams(has_side_effects=True, vmem_limit_bytes=56 * 1024 * 1024),
    )(
        mix_ratio, query_one, key_one, query_two, key_two, values, head_gain.reshape(1, -1), cotangent.T,
        left_roots, right_roots, weight, momentum,
    )
    momentum_new = momentum_decay * momentum + (1.0 - momentum_decay) * prec
    update_step = factor * momentum_new + weight_decay * weight
    weight_new = weight - step_rate * update_step
    return (update_step, weight_new, momentum_new, gathered)


def solution(mesh):
    in_specs = (
        P("fs", "tp"),
        P("fs", "tp"),
        P("fs", "tp"),
        P("fs", "tp"),
        P("fs", "tp"),
        P("tp"),
        P(),
        P("fs", "tp"),
        P("fs", None),
        P("tp", None),
        P("fs", "tp"),
        P("fs", "tp"),
    )
    out_specs = (P("fs", "tp"), P("fs", "tp"), P("fs", "tp"), P(None, "tp"))
    body = functools.partial(local, mesh.shape["fs"], mesh.shape["tp"])
    return jax.shard_map(body, mesh=mesh, in_specs=in_specs, out_specs=out_specs, check_vma=False)
```
